32 devices in a mesh: sp: 4 (over y, x), tp: 8 (over z, core).
Axes of the slice: x: 2, y: 2, z: 4, core: 2. Of those that a mesh axis runs over, the one named last changes fastest.
Arguments:
- queries: bfloat16 [2048, 2048], P('sp', 'tp'), may hold values from -16 to 16
- key_vectors: bfloat16 [2048, 2048], P('sp', 'tp'), may hold values from -4 to 4
- value_vectors: bfloat16 [2048, 2048], P('sp', 'tp'), may hold values from -5 to 5
- forget_totals: float32 [2048, 16], P('sp', 'tp'), may hold values from -344 to 0, as said below
- head_gain: float32 [2048], P('tp'), may hold values from 0.1 to 1.9
- stream: bfloat16 [2048, 2048], P(('sp', 'tp')), may hold values from -6 to 6
- out_weight: bfloat16 [2048, 2048], replicated, may hold values from -0.125 to 0.125
- norm_gain: float32 [2048], replicated, may hold values from 0.1 to 1.9
- routing: int32 [2048, 2], P(('sp', 'tp')), may hold values from 0 to 3, all different within a row; in each aligned block of 64 rows (0 to 63, 64 to 127, ...) at most 64 rows name the same one
- route_weights: float32 [2048, 2], P(('sp', 'tp')), may hold values from 0.2 to 1
- gate_weight: bfloat16 [4, 2048, 4096], P('sp', None, 'tp'), may hold values from -0.125 to 0.125
- up_weight: bfloat16 [4, 2048, 4096], P('sp', None, 'tp'), may hold values from -0.125 to 0.125
- down_weight: bfloat16 [4, 4096, 2048], P('sp', 'tp'), may hold values from -0.09375 to 0.09375
Outputs:
- layer_out: bfloat16 [2048, 2048], P(('sp', 'tp'))
The draws below stay inside these ranges and needn't reach their ends.
Inputs may be any that keep to these rules, and one draw needn't show every extreme that they name: `forget_totals`: along the positions, the values of each head never rise. `routing`: A token's 2 experts differ. Within the tokens of one device (aligned blocks of 64 rows) no expert is named more than 64 times.
All inputs are finite; a program needn't handle non-finite values.
Results may differ from the reference program's by a relative error of at most 0.01145.
Values may be sent and summed in bfloat16 or wider, within the bound.
A program may use at most 128 MiB of HBM per device.

```python
import math
import jax
import jax.numpy as jnp
import numpy as np
from jax import lax

D = 2048
HEAD_COUNT = 16
HD = 128
FF_E = 4096
TOP = 2
TOK_DEV = 512
SEQUENCE_TOKENS = 2048
EXPERTS = 4
ROWS_DEV = 64
CAP = 64
N_TP = 8


def draw_queries(key, part):
    own_key = jax.random.fold_in(key, 11)
    entries = jnp.clip(jax.random.normal(own_key, (SEQUENCE_TOKENS, HEAD_COUNT * HD), jnp.float32), -4.0, 4.0)
    return entries.astype(jnp.bfloat16)


def draw_key_vectors(key, part):
    own_key = jax.random.fold_in(key, 13)
    entries = jnp.clip(jax.random.normal(own_key, (SEQUENCE_TOKENS, HEAD_COUNT * HD), jnp.float32), -4.0, 4.0)
    return entries.astype(jnp.bfloat16)


def draw_forget_totals(key, part):
    ranking = jax.random.permutation(jax.random.fold_in(key, 21), HEAD_COUNT)
    slow_heads = ranking < HEAD_COUNT // 2
    slow_rate = jax.random.uniform(jax.random.fold_in(key, 22), (HEAD_COUNT,), jnp.float32, 0.3, 0.8) / SEQUENCE_TOKENS
    fast_rate = jnp.exp(-jax.random.uniform(jax.random.fold_in(key, 23), (HEAD_COUNT,), jnp.float32, math.log(30.0), math.log(100.0)))
    head_rate = jnp.where(slow_heads, slow_rate, fast_rate)
    block_factor = jnp.exp(jax.random.uniform(jax.random.fold_in(key, 24), (SEQUENCE_TOKENS // TOK_DEV, HEAD_COUNT), jnp.float32, math.log(0.5), math.log(1.5)))
    block_factor = jnp.repeat(block_factor, TOK_DEV, axis=0)
    step_factor = jnp.exp(jax.random.uniform(jax.random.fold_in(key, 25), (SEQUENCE_TOKENS, HEAD_COUNT), jnp.float32, math.log(0.3), math.log(3.0)))
    gate_logarithms = -head_rate[None, :] * block_factor * step_factor
    cluster_positions = jax.random.randint(jax.random.fold_in(key, 26), (3,), 0, SEQUENCE_TOKENS)
    cluster_sizes = jnp.log(jax.random.uniform(jax.random.fold_in(key, 27), (3, HEAD_COUNT), jnp.float32, 0.5, 0.8))
    gate_logarithms = gate_logarithms.at[cluster_positions].add(cluster_sizes)
    return jnp.cumsum(gate_logarithms, axis=0).astype(jnp.float32)


def block_scale(key, dims, shards, least, largest):
    gain = 1.0
    for axis_at, blocks in shards:
        steps = jax.random.uniform(jax.random.fold_in(jax.random.fold_in(key, 6), axis_at), (blocks,), jnp.float32, least / len(shards), largest / len(shards))
        gain = gain * jnp.repeat(jnp.exp(steps), dims[axis_at] // blocks).reshape((-1,) + (1,) * (len(dims) - 1 - axis_at))
    return gain


def routed_block(stream_key, own, number, rows, amount, top, bound, skew):
    sequence = jax.random.permutation(stream_key, amount)
    heavy_load, usual = portions_of(amount, rows * top, bound, skew, True), portions_of(amount, rows * top, bound, skew, False)
    places = jnp.arange(amount)

    def named(lengths, rotation):
        used = int((lengths > 0).sum())
        fixed = max(1, used // 4)
        shifted = fixed + (places - fixed + rotation * (used - fixed)) % max(1, amount - fixed)
        return jnp.zeros((amount,), jnp.int32).at[sequence[jnp.where(places < fixed, places, shifted)]].set(jnp.asarray(lengths, jnp.int32))

    lengths = jnp.where(number % 4 == 0, named(heavy_load, number // 4), named(usual, number - number // 4 - 1))
    mixed = jax.random.permutation(jax.random.fold_in(own, 3), amount)
    donor, receiver = mixed[0:amount // 2 * 2:2], mixed[1:amount // 2 * 2:2]
    slack = jnp.minimum(lengths[donor] - 1, bound - lengths[receiver]) // 2
    slack = jnp.where((donor == sequence[0]) | (receiver == sequence[0]) | (lengths[receiver] == 0), 0, jnp.maximum(slack, 0))
    shifted = jax.random.randint(jax.random.fold_in(own, 4), (amount // 2,), 0, 1 << 20) % (slack + 1)
    lengths = lengths.at[donor].add(-shifted).at[receiver].add(shifted)
    labels = jnp.searchsorted(jnp.cumsum(lengths), jnp.arange(rows * top), side="right").astype(jnp.int32)
    table = labels.reshape(top, rows).T
    table = table[jax.random.permutation(jax.random.fold_in(own, 1), rows)]
    rotation = jax.random.randint(jax.random.fold_in(own, 2), (rows, 1), 0, top)
    return jnp.take_along_axis(table, (jnp.arange(top)[None, :] + rotation) % top, axis=1)


def portions_of(number_of, total, most, slope, full):
    weights = [(1 << 20) // math.isqrt(rank ** slope) + 1 for rank in range(1, number_of + 1)]
    largest = most if full else min(most, max(-(-total // number_of), total * weights[0] // sum(weights)))
    least = 1 if total - largest >= number_of - 1 else 0
    given, spare = [largest] + [least] * (number_of - 1), total - largest - least * (number_of - 1)
    while spare > 0:
        free = [i for i in range(1, number_of) if given[i] < largest] or [i for i in range(1, number_of) if given[i] < most]
        pool, budget = sum([weights[i] for i in free]), spare
        for i in free:
            addition = min(most - given[i], max(1, budget * weights[i] // pool), spare)
            given[i] = given[i] + addition
            spare = spare - addition
    return np.array(given)


def bell_draw(stream_key, dims, spread, bound, split=(), held_as=jnp.bfloat16):
    factor_of = block_scale(stream_key, dims, split, -0.22, 0.18) if split else 1.0
    values = jax.random.normal(stream_key, dims, jnp.float32) * spread * factor_of
    return jnp.minimum(jnp.maximum(values, -bound), bound).astype(held_as)


def setup_inputs(seed: int = 0) -> dict:
    seeds = jax.random.split(jax.random.key(seed), 14)
    queries = draw_queries(jax.random.fold_in(seeds[13], 71), 0)
    key_vectors = draw_key_vectors(jax.random.fold_in(seeds[13], 71), 0)
    value_vectors = bell_draw(seeds[2], (SEQUENCE_TOKENS, HEAD_COUNT * HD), 1.0, 5.0, ((0, 4), (1, 8)))
    forget_totals = draw_forget_totals(jax.random.fold_in(seeds[13], 71), 0)
    head_gain = jnp.clip(1.0 + 0.18 * jax.random.normal(seeds[4], (HEAD_COUNT * HD,), jnp.float32), 0.1, 1.9)
    stream = bell_draw(seeds[5], (SEQUENCE_TOKENS, D), 1.0, 6.0, ((0, 32),))
    out_weight = bell_draw(seeds[6], (HEAD_COUNT * HD, D), (HEAD_COUNT * HD) ** -0.5, 0.125)
    norm_gain = jnp.clip(1.0 + 0.18 * jax.random.normal(seeds[7], (D,), jnp.float32), 0.1, 1.9)
    routing_keys = jax.random.split(jax.random.fold_in(seeds[8], 1), SEQUENCE_TOKENS // ROWS_DEV)
    routing_turns = jax.random.permutation(jax.random.fold_in(seeds[8], 3), SEQUENCE_TOKENS // ROWS_DEV)
    routing = jax.vmap(lambda own, number: routed_block(jax.random.fold_in(seeds[8], 2), own, number, ROWS_DEV, EXPERTS, TOP, CAP, 1))(routing_keys, routing_turns).reshape((SEQUENCE_TOKENS, TOP))
    route_weights = jnp.clip(0.2 + 0.8 * jax.random.uniform(seeds[9], (SEQUENCE_TOKENS, TOP), jnp.float32) ** block_scale(seeds[9], (SEQUENCE_TOKENS, TOP), ((0, 32),), -0.2, 0.2), 0.2, 1.0)
    gate_weight = bell_draw(seeds[10], (EXPERTS, D, FF_E), D ** -0.5, 0.125, ((0, 4), (2, 8)))
    up_weight = bell_draw(seeds[11], (EXPERTS, D, FF_E), D ** -0.5, 0.125, ((0, 4), (2, 8)))
    down_weight = bell_draw(seeds[12], (EXPERTS, FF_E, D), FF_E ** -0.5, 0.09375, ((0, 4), (1, 8)))
    return {"queries": queries, "key_vectors": key_vectors, "value_vectors": value_vectors, "forget_totals": forget_totals, "head_gain": head_gain, "stream": stream, "out_weight": out_weight, "norm_gain": norm_gain, "routing": routing, "route_weights": route_weights, "gate_weight": gate_weight, "up_weight": up_weight, "down_weight": down_weight}


def attention_rows(queries, key_vectors, value_vectors, forget_totals, head_gain):
    seq_len = queries.shape[0]
    query_block = 512 if seq_len % 512 == 0 else seq_len
    query_complete = queries.astype(jnp.float32).reshape(seq_len, HEAD_COUNT, HD)
    key_all = key_vectors.astype(jnp.float32).reshape(seq_len, HEAD_COUNT, HD)
    value_all = value_vectors.astype(jnp.float32).reshape(seq_len, HEAD_COUNT, HD)
    gate_rows = jnp.transpose(forget_totals)
    key_pos = jnp.arange(seq_len, dtype=jnp.int32)
    gain_grid = head_gain.reshape(HEAD_COUNT, 1, HD)

    def one_block(block_index):
        first_row = block_index * query_block
        query_rows = lax.dynamic_slice_in_dim(query_complete, first_row, query_block, 0)
        query_gate = lax.dynamic_slice_in_dim(gate_rows, first_row, query_block, 1)
        scores = jnp.einsum('qhd,khd->hqk', query_rows, key_all) * HD ** (-0.5) + query_gate[:, :, None] - gate_rows[:, None, :]
        query_pos = first_row + jnp.arange(query_block, dtype=jnp.int32)
        visible = (key_pos[None, :] <= query_pos[:, None])[None]
        scores = jnp.where(visible, scores, -jnp.inf)
        row_peak = lax.optimization_barrier(jnp.max(scores, axis=2, keepdims=True))
        lifted = jnp.exp(scores - row_peak)
        row_total = lax.optimization_barrier(jnp.sum(lifted, axis=2))
        rounded = lax.optimization_barrier(lifted.astype(jnp.bfloat16))
        numerator = jnp.einsum('hqk,khd->hqd', rounded.astype(jnp.float32), value_all)
        attended = numerator / row_total[:, :, None]
        inverse_rms = lax.rsqrt(lax.optimization_barrier(jnp.mean(attended * attended, axis=2, keepdims=True)) + 1e-06)
        normed = attended * inverse_rms * gain_grid
        return jnp.transpose(normed, (1, 0, 2)).reshape(query_block, HEAD_COUNT * HD).astype(jnp.bfloat16)
    block_count = seq_len // query_block
    head_out = lax.map(one_block, jnp.arange(block_count, dtype=jnp.int32))
    return head_out.reshape(seq_len, HEAD_COUNT * HD)

def expert_rows(normed_rows, routing, route_weights, gate_weight, up_weight, down_weight):
    token_count = normed_rows.shape[0]
    row_block = 128
    flat_expert = routing.reshape(-1).astype(jnp.int32)
    pair_count = flat_expert.shape[0]
    flat_token = (jnp.arange(pair_count, dtype=jnp.int32) // TOP).astype(jnp.int32)
    flat_weight = route_weights.reshape(-1)
    ordering = jnp.argsort(flat_expert, stable=True)
    sorted_expert = flat_expert[ordering]
    per_expert = lax.optimization_barrier(jnp.sum((flat_expert[:, None] == jnp.arange(EXPERTS, dtype=jnp.int32)[None, :]).astype(jnp.int32), axis=0)).astype(jnp.int32)
    padded = ((per_expert + row_block - 1) // row_block * row_block).astype(jnp.int32)
    pad_end = jnp.cumsum(padded).astype(jnp.int32)
    pad_start = (pad_end - padded).astype(jnp.int32)
    run_start = (jnp.cumsum(per_expert) - per_expert).astype(jnp.int32)
    target = (pad_start[sorted_expert] + jnp.arange(pair_count, dtype=jnp.int32) - run_start[sorted_expert]).astype(jnp.int32)
    block_count = -(-pair_count // row_block) + EXPERTS
    slot_total = block_count * row_block
    slot_token = jnp.full((slot_total,), token_count, jnp.int32).at[target].set(flat_token[ordering])
    slot_weight = jnp.zeros((slot_total,), jnp.float32).at[target].set(flat_weight[ordering])
    block_starts = (jnp.arange(block_count, dtype=jnp.int32) * row_block).astype(jnp.int32)
    block_expert = jnp.minimum(jnp.searchsorted(pad_end, block_starts, side='right').astype(jnp.int32), EXPERTS - 1).astype(jnp.int32)
    padded_rows = jnp.concatenate([normed_rows, jnp.zeros((1, normed_rows.shape[1]), normed_rows.dtype)], axis=0)[slot_token]
    units_dev = FF_E // N_TP

    def expert_block(block_args):
        block_in, expert_id = block_args
        gate_pre = jnp.dot(block_in, gate_weight[expert_id], preferred_element_type=jnp.float32)
        up_pre = jnp.dot(block_in, up_weight[expert_id], preferred_element_type=jnp.float32)
        hidden = lax.optimization_barrier((jax.nn.silu(gate_pre) * up_pre).astype(jnp.bfloat16))
        grouped_rows = jnp.transpose(hidden.reshape(row_block, N_TP, units_dev), (1, 0, 2)).astype(jnp.float32)
        down_groups = down_weight[expert_id].reshape(N_TP, units_dev, -1).astype(jnp.float32)
        partial_value = lax.optimization_barrier(jnp.einsum('gbf,gfd->gbd', grouped_rows, down_groups).astype(jnp.bfloat16))
        return lax.optimization_barrier(jnp.sum(partial_value.astype(jnp.float32), axis=0)).astype(jnp.bfloat16)
    expert_out = lax.map(expert_block, (padded_rows.reshape(block_count, row_block, -1), block_expert))
    expert_out = expert_out.reshape(slot_total, -1)
    weighted = expert_out.astype(jnp.float32) * slot_weight[:, None]
    return jax.ops.segment_sum(weighted, slot_token, num_segments=token_count + 1)[:token_count]

def reference(queries, key_vectors, value_vectors, forget_totals, head_gain, stream, out_weight, norm_gain, routing, route_weights, gate_weight, up_weight, down_weight):
    head_out = attention_rows(queries, key_vectors, value_vectors, forget_totals, head_gain)
    mixed_rows = jnp.dot(head_out, out_weight, preferred_element_type=jnp.float32)
    resid_sum = stream.astype(jnp.float32) + mixed_rows
    center = resid_sum - lax.optimization_barrier(jnp.mean(resid_sum, axis=1, keepdims=True))
    normed_rows = (center * lax.rsqrt(lax.optimization_barrier(jnp.mean(center * center, axis=1, keepdims=True)) + 1e-05) * norm_gain).astype(jnp.bfloat16)
    routed = expert_rows(normed_rows, routing, route_weights, gate_weight, up_weight, down_weight)
    return (resid_sum + routed).astype(jnp.bfloat16)
```

```python
from functools import partial

import jax
import jax.numpy as jnp
from jax import lax
from jax.experimental import pallas as pl
from jax.experimental.pallas import tpu as pltpu
from jax.sharding import PartitionSpec as P

HD = 128
TOP = 2


masked_score = -1e30


def attend_block(
    totals, query_rows, query_gate, query_pos, key_rows, value_rows, key_gate, key_pos
):
    run_max, run_sum, run_acc = totals
    scores = jnp.einsum("qhd,khd->hqk", query_rows, key_rows, preferred_element_type=jnp.float32)
    scores = scores * HD ** (-0.5) + query_gate[:, :, None] - key_gate[:, None, :]
    visible = (key_pos[None, :] <= query_pos[:, None])[None]
    scores = jnp.where(visible, scores, masked_score)
    new_max = jnp.maximum(run_max, jnp.max(scores, axis=2))
    lifted = jnp.where(visible, jnp.exp(scores - new_max[:, :, None]), 0.0)
    rescale = jnp.exp(run_max - new_max)
    new_sum = run_sum * rescale + jnp.sum(lifted, axis=2)
    product = jnp.einsum(
        "hqk,khd->hqd", lifted.astype(jnp.bfloat16), value_rows, preferred_element_type=jnp.float32
    )
    new_acc = run_acc * rescale[:, :, None] + product
    return (new_max, new_sum, new_acc)


def keep_totals(totals_in):
    return totals_in


def make_folder(segments, gathered_gates):

    def fold_keys(state_all, key_piece, first_key):
        key_part, value_part = key_piece
        key_total = key_part.shape[0]
        block_len = min(512, key_total)
        heads_dev = segments[0][0].shape[1]
        key_part = key_part.reshape(key_total, heads_dev, HD)
        value_part = value_part.reshape(key_total, heads_dev, HD)

        def one_block(block_index, state_now):
            offset = block_index * block_len
            key_rows = lax.dynamic_slice_in_dim(key_part, offset, block_len, 0)
            value_rows = lax.dynamic_slice_in_dim(value_part, offset, block_len, 0)
            key_pos = offset + jnp.arange(block_len, dtype=jnp.int32)
            key_gate = jnp.transpose(lax.dynamic_slice_in_dim(gathered_gates, offset, block_len, 0))
            updated = []
            for segment, totals_in in zip(segments, state_now):
                query_rows, query_gate, query_pos = segment
                needed = offset <= query_pos[-1]
                advance = partial(
                    attend_block,
                    query_rows=query_rows,
                    query_gate=query_gate,
                    query_pos=query_pos,
                    key_rows=key_rows,
                    value_rows=value_rows,
                    key_gate=key_gate,
                    key_pos=key_pos,
                )
                updated.append(lax.cond(needed, advance, keep_totals, totals_in))
            return tuple(updated)

        return lax.fori_loop(0, key_total // block_len, one_block, state_all)

    return fold_keys


MESH = pl.DeviceIdType.MESH
LANES = 128
QUADS = 4


def z_steps(depth):
    steps = []
    for near in range(1, depth // 2 + 1):
        for step in (near, depth - near):
            if step not in steps:
                steps.append(step)
    return steps


def experts_kernel(
    depth,
    own_rows,
    resid,
    gate_hbm,
    up_hbm,
    down_hbm,
    out_ref,
    rows_all,
    gate_w,
    up_w,
    down_w,
    hidden,
    mine,
    theirs,
    from_core,
    from_second,
    from_first,
    from_z,
    local_sems,
    ag_send_sems,
    ag_recv_sems,
    rs_send_sems,
    core_sems,
    second_sems,
    first_sems,
    z_sems,
):
    sp = lax.axis_index("sp")
    tp = lax.axis_index("tp")
    width = resid.shape[1]
    count = resid.shape[0]
    z, core = tp // 2, tp % 2
    other = 1 - core
    x_next = sp + 1 - 2 * (sp % 2)
    y_next = (sp + 2) % 4
    first = x_next * (1 - core) + y_next * core
    second = y_next * (1 - core) + x_next * core
    far = 3 - sp
    to_core = (sp, z * 2 + other)
    to_first = (first, tp)
    to_second = (second, tp)

    def to_z(step):
        return (sp, ((z + step) % depth) * 2 + core)

    steps = z_steps(depth)
    loads = [
        pltpu.make_async_copy(own_rows, rows_all.at[core * QUADS + sp, z], local_sems.at[0]),
        pltpu.make_async_copy(gate_hbm.at[0], gate_w, local_sems.at[1]),
        pltpu.make_async_copy(up_hbm.at[0], up_w, local_sems.at[2]),
        pltpu.make_async_copy(down_hbm.at[0], down_w, local_sems.at[3]),
    ]
    for load in loads:
        load.start()

    barrier = pltpu.get_barrier_semaphore()
    peers = [to_core, to_first, to_second] + [to_z(step) for step in steps]
    for peer in peers:
        pl.semaphore_signal(barrier, inc=1, device_id=peer, device_id_type=MESH)
    pl.semaphore_wait(barrier, len(peers))

    started = []

    def spread(src, group, zz, target):
        copy = pltpu.make_async_remote_copy(
            src_ref=src,
            dst_ref=rows_all.at[group, zz],
            send_sem=ag_send_sems.at[len(started)],
            recv_sem=ag_recv_sems.at[group, zz],
            device_id=target,
            device_id_type=MESH,
        )
        copy.start()
        started.append(copy)

    def arrived(group, zz):
        slot = rows_all.at[group, zz]
        pltpu.make_async_remote_copy(
            src_ref=slot,
            dst_ref=slot,
            send_sem=ag_send_sems.at[0],
            recv_sem=ag_recv_sems.at[group, zz],
            device_id=to_core,
            device_id_type=MESH,
        ).wait_recv()

    def onward(group, zz, targets):
        arrived(group, zz)
        for target in targets:
            spread(rows_all.at[group, zz], group, zz, target)

    def from_partner(quad):
        for zz in range(depth):
            arrived(other * QUADS + quad, zz)

    def experts(group, dest, quad):
        half = 256 if gate_w.shape[1] % 256 == 0 else gate_w.shape[1]

        @pl.loop(0, gate_w.shape[1] // half)
        def _(j):
            cols = pl.ds(pl.multiple_of(j * half, half), half)
            block = rows_all[group, :, :, :width].reshape(depth * count, width)
            gate_pre = jnp.dot(block, gate_w[:, cols], preferred_element_type=jnp.float32)
            up_pre = jnp.dot(block, up_w[:, cols], preferred_element_type=jnp.float32)
            hidden[:, cols] = (gate_pre / (1.0 + jnp.exp(-gate_pre)) * up_pre).astype(jnp.bfloat16)

        pieces = rows_all[group, :, :, width:].reshape(depth * count, LANES).astype(jnp.float32)
        lane = lax.broadcasted_iota(jnp.int32, pieces.shape, 1)
        weight = jnp.sum(jnp.where(lane % QUADS == sp, pieces, 0.0), axis=1, keepdims=True)
        step = 512 if width % 512 == 0 else width

        @pl.loop(0, width // step)
        def _(j):
            cols = pl.ds(pl.multiple_of(j * step, step), step)
            product = jnp.dot(hidden[...], down_w[:, cols], preferred_element_type=jnp.float32)
            dest[quad, :, :, cols] = (
                (product * weight).astype(jnp.bfloat16).reshape(depth, count, step)
            )

    returned = []

    def send_back(src, dst, sem, target):
        copy = pltpu.make_async_remote_copy(
            src_ref=src,
            dst_ref=dst,
            send_sem=rs_send_sems.at[len(returned)],
            recv_sem=sem,
            device_id=target,
            device_id_type=MESH,
        )
        copy.start()
        returned.append(copy)

    def landed(dst, sem):
        pltpu.make_async_remote_copy(
            src_ref=dst,
            dst_ref=dst,
            send_sem=rs_send_sems.at[0],
            recv_sem=sem,
            device_id=to_core,
            device_id_type=MESH,
        ).wait_recv()

    def partner_part(quad):
        experts(other * QUADS + quad, theirs, quad)
        send_back(theirs.at[quad], from_core.at[quad], core_sems.at[quad], to_core)

    def f32(value):
        return value.astype(jnp.float32)

    own_group = core * QUADS + sp
    for target in [to_z(step) for step in steps] + [to_first, to_second, to_core]:
        spread(own_rows, own_group, z, target)
    before = None
    for step in [0] + steps + [None]:
        if step:
            onward(own_group, (z - step + depth) % depth, [to_first, to_second, to_core])
        if before is not None:
            zz = (z - before + depth) % depth
            onward(core * QUADS + first, zz, [to_second, to_core])
        before = step
    for load in loads:
        load.wait()
    order = [0] + steps
    experts(own_group, mine, sp)
    from_partner(sp)
    partner_part(sp)
    for step in order:
        onward(core * QUADS + second, (z - step + depth) % depth, [to_core])
    experts(core * QUADS + first, mine, first)
    from_partner(second)
    partner_part(second)
    experts(core * QUADS + second, mine, second)
    from_partner(first)
    partner_part(first)

    back_steps = steps + [0]

    def hand_over(quad, slot):
        landed(from_core.at[quad], core_sems.at[quad])
        mine[quad] = (f32(mine[quad]) + f32(from_core[quad])).astype(jnp.bfloat16)
        for step in back_steps:
            zz = (z + step) % depth
            send_back(
                mine.at[quad, zz], from_second.at[slot, zz], second_sems.at[slot, zz], to_second
            )

    hand_over(second, 0)
    for step in order:
        onward(core * QUADS + far, (z - step + depth) % depth, [to_core])
    experts(core * QUADS + far, mine, far)
    from_partner(far)
    partner_part(far)
    hand_over(far, 1)

    landed(from_core.at[first], core_sems.at[first])
    landed(from_core.at[sp], core_sems.at[sp])
    for step in back_steps:
        zz = (z + step) % depth
        landed(from_second.at[1, zz], second_sems.at[1, zz])
        mine[first, zz] = (
            f32(mine[first, zz]) + f32(from_core[first, zz]) + f32(from_second[1, zz])
        ).astype(jnp.bfloat16)
        send_back(mine.at[first, zz], from_first.at[zz], first_sems.at[zz], to_first)
    for step in back_steps:
        zz = (z + step) % depth
        landed(from_second.at[0, zz], second_sems.at[0, zz])
        landed(from_first.at[zz], first_sems.at[zz])
        total = (
            f32(mine[sp, zz])
            + f32(from_core[sp, zz])
            + f32(from_second[0, zz])
            + f32(from_first[zz])
        )
        if step:
            mine[sp, zz] = total.astype(jnp.bfloat16)
            send_back(mine.at[sp, zz], from_z.at[step - 1], z_sems.at[step - 1], to_z(step))
        else:
            total = resid[...] + total
            for slot in range(depth - 1):
                landed(from_z.at[slot], z_sems.at[slot])
                total = total + f32(from_z[slot])
            out_ref[...] = total.astype(out_ref.dtype)
    for copy in started + returned:
        copy.wait_send()


def dense_experts(
    resid_sum, normed_rows, routing, route_weights, gate_weight, up_weight, down_weight
):
    depth = lax.axis_size("tp") // 2
    count, width = normed_rows.shape
    units = gate_weight.shape[2]
    experts = jnp.arange(QUADS, dtype=jnp.int32)
    named = routing[:, :, None] == experts[None, None, :]
    weights = jnp.sum(jnp.where(named, route_weights[:, :, None], 0.0), axis=1)
    high = lax.reduce_precision(weights, 8, 7)
    middle = lax.reduce_precision(weights - high, 8, 7)
    low = weights - high - middle
    pieces = jnp.concatenate([high, middle, low], axis=1).astype(jnp.bfloat16)
    pieces = jnp.pad(pieces, ((0, 0), (0, LANES - pieces.shape[1])))
    extended = jnp.concatenate([normed_rows, pieces], axis=1)
    bf16 = jnp.bfloat16
    dma = pltpu.SemaphoreType.DMA
    block = (depth, count, width)
    vmem = pl.BlockSpec(memory_space=pltpu.VMEM)
    hbm = pl.BlockSpec(memory_space=pl.ANY)
    ag_sends = (depth - 1 + 3) + 3 * (depth - 1) + 2 * depth + 2 * depth
    rs_sends = QUADS + 2 * depth + depth + depth - 1
    return pl.pallas_call(
        partial(experts_kernel, depth),
        out_shape=jax.ShapeDtypeStruct((count, width), bf16),
        in_specs=[vmem, vmem, hbm, hbm, hbm],
        out_specs=vmem,
        scratch_shapes=[
            pltpu.VMEM((2 * QUADS, depth, count, width + LANES), bf16),
            pltpu.VMEM((width, units), bf16),
            pltpu.VMEM((width, units), bf16),
            pltpu.VMEM((units, width), bf16),
            pltpu.VMEM((depth * count, units), bf16),
            pltpu.VMEM((QUADS,) + block, bf16),
            pltpu.VMEM((QUADS,) + block, bf16),
            pltpu.VMEM((QUADS,) + block, bf16),
            pltpu.VMEM((2,) + block, bf16),
            pltpu.VMEM(block, bf16),
            pltpu.VMEM((depth - 1, count, width), bf16),
            dma((4,)),
            dma((ag_sends,)),
            dma((2 * QUADS, depth)),
            dma((rs_sends,)),
            dma((QUADS,)),
            dma((2, depth)),
            dma((depth,)),
            dma((depth - 1,)),
        ],
        compiler_params=pltpu.CompilerParams(
            collective_id=0, has_side_effects=True, vmem_limit_bytes=48 * 2**20
        ),
    )(extended, resid_sum, gate_weight, up_weight, down_weight)


def routed_experts(
    resid_sum, normed_rows, routing, route_weights, gate_weight, up_weight, down_weight
):
    sp_count = lax.axis_size("sp")
    row_count = normed_rows.shape[0]
    capacity = max(2, 2 * TOP * row_count // sp_count)
    flat_expert = routing.reshape(-1)
    onehot = (flat_expert[:, None] == jnp.arange(sp_count, dtype=jnp.int32)[None, :]).astype(
        jnp.int32
    )
    earlier = jnp.cumsum(onehot, axis=0) - onehot
    slot_index = flat_expert * capacity + jnp.sum(earlier * onehot, axis=1)
    slot_grid = slot_index.reshape(row_count, TOP)
    slot_ids = jnp.arange(sp_count * capacity, dtype=jnp.int32)
    placing = jnp.sum(
        (slot_grid[None, :, :] == slot_ids[:, None, None]).astype(jnp.float32), axis=2
    ).astype(jnp.bfloat16)
    outgoing = jnp.dot(placing, normed_rows, preferred_element_type=jnp.float32).astype(
        jnp.bfloat16
    )
    outgoing = outgoing.reshape(sp_count, capacity, normed_rows.shape[1])
    arrived = lax.all_to_all(outgoing, "sp", split_axis=0, concat_axis=0, tiled=True)
    row_piece = lax.all_gather(arrived.reshape(-1, arrived.shape[2]), "tp", axis=0, tiled=True)
    gate_pre = jnp.dot(row_piece, gate_weight[0], preferred_element_type=jnp.float32)
    up_pre = jnp.dot(row_piece, up_weight[0], preferred_element_type=jnp.float32)
    hidden = (jax.nn.silu(gate_pre) * up_pre).astype(jnp.bfloat16)
    summed = lax.psum_scatter(
        jnp.dot(hidden, down_weight[0], preferred_element_type=jnp.float32).astype(jnp.bfloat16),
        "tp",
        scatter_dimension=0,
        tiled=True,
    )
    expert_out = summed.reshape(sp_count, capacity, -1)
    returned = lax.all_to_all(expert_out, "sp", split_axis=0, concat_axis=0, tiled=True)
    picked = returned.reshape(sp_count * capacity, -1)[slot_index].astype(jnp.float32)
    weighted = picked * route_weights.reshape(-1)[:, None]
    routed = jnp.sum(weighted.reshape(row_count, TOP, -1), axis=1)
    return (resid_sum + routed).astype(jnp.bfloat16)


def on_device(
    queries,
    key_vectors,
    value_vectors,
    forget_totals,
    head_gain,
    stream,
    out_weight,
    norm_gain,
    routing,
    route_weights,
    gate_weight,
    up_weight,
    down_weight,
):
    tok_count = queries.shape[0]
    heads_dev = queries.shape[1] // HD
    sp_index = lax.axis_index("sp")
    sp_count = lax.axis_size("sp")
    gathered_gates = lax.all_gather(forget_totals, "sp", axis=0, tiled=True)
    first_pos = sp_index * tok_count
    query_pos = first_pos + jnp.arange(tok_count, dtype=jnp.int32)
    query_gate = jnp.transpose(lax.dynamic_slice_in_dim(gathered_gates, first_pos, tok_count, 0))
    segments = [(queries.reshape(tok_count, heads_dev, HD), query_gate, query_pos)]
    starting = (
        (
            jnp.full((heads_dev, tok_count), masked_score, jnp.float32),
            jnp.zeros((heads_dev, tok_count), jnp.float32),
            jnp.zeros((heads_dev, tok_count, HD), jnp.float32),
        ),
    )
    folder = make_folder(segments, gathered_gates)
    totals = folder(
        starting,
        (
            lax.all_gather(key_vectors, "sp", axis=0, tiled=True),
            lax.all_gather(value_vectors, "sp", axis=0, tiled=True),
        ),
        jnp.int32(0),
    )
    run_max, run_sum, run_acc = totals[0]
    attended = run_acc / run_sum[:, :, None]
    inverse_rms = lax.rsqrt(jnp.mean(attended * attended, axis=2, keepdims=True) + 1e-06)
    normed = attended * inverse_rms * head_gain.reshape(heads_dev, 1, HD)
    head_out = (
        jnp.transpose(normed, (1, 0, 2)).reshape(tok_count, heads_dev * HD).astype(jnp.bfloat16)
    )
    token_heads = lax.all_to_all(head_out, "tp", split_axis=0, concat_axis=1, tiled=True)
    mixed_rows = jnp.dot(token_heads, out_weight, preferred_element_type=jnp.float32)
    resid_sum = stream.astype(jnp.float32) + mixed_rows
    center = resid_sum - jnp.mean(resid_sum, axis=1, keepdims=True)
    normed_rows = (
        center * lax.rsqrt(jnp.mean(center * center, axis=1, keepdims=True) + 1e-05) * norm_gain
    ).astype(jnp.bfloat16)
    row_count = normed_rows.shape[0]
    if sp_count == QUADS and lax.axis_size("tp") % 4 == 0 and 2 * TOP * row_count // sp_count >= row_count:
        return dense_experts(
            resid_sum, normed_rows, routing, route_weights, gate_weight, up_weight, down_weight
        )
    return routed_experts(
        resid_sum, normed_rows, routing, route_weights, gate_weight, up_weight, down_weight
    )


def solution(mesh):
    in_specs = (
        P("sp", "tp"),
        P("sp", "tp"),
        P("sp", "tp"),
        P("sp", "tp"),
        P("tp"),
        P(("sp", "tp"), None),
        P(),
        P(),
        P(("sp", "tp"), None),
        P(("sp", "tp"), None),
        P("sp", None, "tp"),
        P("sp", None, "tp"),
        P("sp", "tp", None),
    )
    out_specs = P(("sp", "tp"), None)
    return jax.shard_map(
        on_device, mesh=mesh, in_specs=in_specs, out_specs=out_specs, check_vma=False
    )
```

```python
from functools import partial

import jax
import jax.numpy as jnp
from jax import lax
from jax.experimental import pallas as pl
from jax.experimental.pallas import tpu as pltpu
from jax.sharding import PartitionSpec as P

HD = 128
TOP = 2


masked_score = -1e30


def attend_block(
    totals, query_rows, query_gate, query_pos, key_rows, value_rows, key_gate, key_pos
):
    run_max, run_sum, run_acc = totals
    scores = jnp.einsum("qhd,khd->hqk", query_rows, key_rows, preferred_element_type=jnp.float32)
    scores = scores * HD ** (-0.5) + query_gate[:, :, None] - key_gate[:, None, :]
    visible = (key_pos[None, :] <= query_pos[:, None])[None]
    scores = jnp.where(visible, scores, masked_score)
    new_max = jnp.maximum(run_max, jnp.max(scores, axis=2))
    lifted = jnp.where(visible, jnp.exp(scores - new_max[:, :, None]), 0.0)
    rescale = jnp.exp(run_max - new_max)
    new_sum = run_sum * rescale + jnp.sum(lifted, axis=2)
    product = jnp.einsum(
        "hqk,khd->hqd", lifted.astype(jnp.bfloat16), value_rows, preferred_element_type=jnp.float32
    )
    new_acc = run_acc * rescale[:, :, None] + product
    return (new_max, new_sum, new_acc)


def keep_totals(totals_in):
    return totals_in


def make_folder(segments, gathered_gates):

    def fold_keys(state_all, key_piece, first_key):
        key_part, value_part = key_piece
        key_total = key_part.shape[0]
        block_len = min(512, key_total)
        heads_dev = segments[0][0].shape[1]
        key_part = key_part.reshape(key_total, heads_dev, HD)
        value_part = value_part.reshape(key_total, heads_dev, HD)

        def one_block(block_index, state_now):
            offset = block_index * block_len
            key_rows = lax.dynamic_slice_in_dim(key_part, offset, block_len, 0)
            value_rows = lax.dynamic_slice_in_dim(value_part, offset, block_len, 0)
            key_pos = offset + jnp.arange(block_len, dtype=jnp.int32)
            key_gate = jnp.transpose(lax.dynamic_slice_in_dim(gathered_gates, offset, block_len, 0))
            updated = []
            for segment, totals_in in zip(segments, state_now):
                query_rows, query_gate, query_pos = segment
                needed = offset <= query_pos[-1]
                advance = partial(
                    attend_block,
                    query_rows=query_rows,
                    query_gate=query_gate,
                    query_pos=query_pos,
                    key_rows=key_rows,
                    value_rows=value_rows,
                    key_gate=key_gate,
                    key_pos=key_pos,
                )
                updated.append(lax.cond(needed, advance, keep_totals, totals_in))
            return tuple(updated)

        return lax.fori_loop(0, key_total // block_len, one_block, state_all)

    return fold_keys


MESH = pl.DeviceIdType.MESH
LANES = 128
QUADS = 4


def z_steps(depth):
    steps = []
    for near in range(1, depth // 2 + 1):
        for step in (near, depth - near):
            if step not in steps:
                steps.append(step)
    return steps


def experts_kernel(
    depth,
    own_rows,
    resid,
    gate_hbm,
    up_hbm,
    down_hbm,
    out_ref,
    rows_all,
    gate_w,
    up_w,
    down_w,
    hidden,
    mine,
    theirs,
    from_core,
    from_second,
    from_first,
    from_z,
    local_sems,
    ag_send_sems,
    ag_recv_sems,
    rs_send_sems,
    core_sems,
    second_sems,
    first_sems,
    z_sems,
):
    sp = lax.axis_index("sp")
    tp = lax.axis_index("tp")
    width = resid.shape[1]
    count = resid.shape[0]
    z, core = tp // 2, tp % 2
    other = 1 - core
    x_next = sp + 1 - 2 * (sp % 2)
    y_next = (sp + 2) % 4
    first = x_next * (1 - core) + y_next * core
    second = y_next * (1 - core) + x_next * core
    far = 3 - sp
    to_core = (sp, z * 2 + other)
    to_first = (first, tp)
    to_second = (second, tp)

    def to_z(step):
        return (sp, ((z + step) % depth) * 2 + core)

    steps = z_steps(depth)
    loads = [
        pltpu.make_async_copy(own_rows, rows_all.at[core * QUADS + sp, z], local_sems.at[0]),
        pltpu.make_async_copy(gate_hbm.at[0], gate_w, local_sems.at[1]),
        pltpu.make_async_copy(up_hbm.at[0], up_w, local_sems.at[2]),
        pltpu.make_async_copy(down_hbm.at[0], down_w, local_sems.at[3]),
    ]
    for load in loads:
        load.start()

    barrier = pltpu.get_barrier_semaphore()
    peers = [to_core, to_first, to_second] + [to_z(step) for step in steps]
    for peer in peers:
        pl.semaphore_signal(barrier, inc=1, device_id=peer, device_id_type=MESH)
    pl.semaphore_wait(barrier, len(peers))

    started = []

    def spread(src, group, zz, target):
        copy = pltpu.make_async_remote_copy(
            src_ref=src,
            dst_ref=rows_all.at[group, zz],
            send_sem=ag_send_sems.at[len(started)],
            recv_sem=ag_recv_sems.at[group, zz],
            device_id=target,
            device_id_type=MESH,
        )
        copy.start()
        started.append(copy)

    def arrived(group, zz):
        slot = rows_all.at[group, zz]
        pltpu.make_async_remote_copy(
            src_ref=slot,
            dst_ref=slot,
            send_sem=ag_send_sems.at[0],
            recv_sem=ag_recv_sems.at[group, zz],
            device_id=to_core,
            device_id_type=MESH,
        ).wait_recv()

    def onward(group, zz, targets):
        arrived(group, zz)
        for target in targets:
            spread(rows_all.at[group, zz], group, zz, target)

    def from_partner(quad):
        for zz in range(depth):
            arrived(other * QUADS + quad, zz)

    def experts(group, dest, quad):
        half = 256 if gate_w.shape[1] % 256 == 0 else gate_w.shape[1]

        @pl.loop(0, gate_w.shape[1] // half)
        def _(j):
            cols = pl.ds(pl.multiple_of(j * half, half), half)
            block = rows_all[group, :, :, :width].reshape(depth * count, width)
            gate_pre = jnp.dot(block, gate_w[:, cols], preferred_element_type=jnp.float32)
            up_pre = jnp.dot(block, up_w[:, cols], preferred_element_type=jnp.float32)
            hidden[:, cols] = (gate_pre / (1.0 + jnp.exp(-gate_pre)) * up_pre).astype(jnp.bfloat16)

        pieces = rows_all[group, :, :, width:].reshape(depth * count, LANES).astype(jnp.float32)
        lane = lax.broadcasted_iota(jnp.int32, pieces.shape, 1)
        weight = jnp.sum(jnp.where(lane % QUADS == sp, pieces, 0.0), axis=1, keepdims=True)
        step = 512 if width % 512 == 0 else width

        @pl.loop(0, width // step)
        def _(j):
            cols = pl.ds(pl.multiple_of(j * step, step), step)
            product = jnp.dot(hidden[...], down_w[:, cols], preferred_element_type=jnp.float32)
            dest[quad, :, :, cols] = (
                (product * weight).astype(jnp.bfloat16).reshape(depth, count, step)
            )

    returned = []

    def send_back(src, dst, sem, target):
        copy = pltpu.make_async_remote_copy(
            src_ref=src,
            dst_ref=dst,
            send_sem=rs_send_sems.at[len(returned)],
            recv_sem=sem,
            device_id=target,
            device_id_type=MESH,
        )
        copy.start()
        returned.append(copy)

    def landed(dst, sem):
        pltpu.make_async_remote_copy(
            src_ref=dst,
            dst_ref=dst,
            send_sem=rs_send_sems.at[0],
            recv_sem=sem,
            device_id=to_core,
            device_id_type=MESH,
        ).wait_recv()

    def partner_part(quad):
        experts(other * QUADS + quad, theirs, quad)
        send_back(theirs.at[quad], from_core.at[quad], core_sems.at[quad], to_core)

    def f32(value):
        return value.astype(jnp.float32)

    own_group = core * QUADS + sp
    for target in [to_z(step) for step in steps] + [to_first, to_second, to_core]:
        spread(own_rows, own_group, z, target)
    before = None
    for step in [0] + steps + [None]:
        if step:
            onward(own_group, (z - step + depth) % depth, [to_first, to_second, to_core])
        if before is not None:
            zz = (z - before + depth) % depth
            onward(core * QUADS + first, zz, [to_second, to_core])
        before = step
    for load in loads:
        load.wait()
    order = [0] + steps
    experts(own_group, mine, sp)
    from_partner(sp)
    partner_part(sp)
    for step in order:
        onward(core * QUADS + second, (z - step + depth) % depth, [to_core])
    experts(core * QUADS + first, mine, first)
    from_partner(second)
    partner_part(second)
    experts(core * QUADS + second, mine, second)
    from_partner(first)
    partner_part(first)

    back_steps = steps + [0]

    def hand_over(quad, slot):
        landed(from_core.at[quad], core_sems.at[quad])
        mine[quad] = (f32(mine[quad]) + f32(from_core[quad])).astype(jnp.bfloat16)
        for step in back_steps:
            zz = (z + step) % depth
            send_back(
                mine.at[quad, zz], from_second.at[slot, zz], second_sems.at[slot, zz], to_second
            )

    hand_over(second, 0)
    for step in order:
        onward(core * QUADS + far, (z - step + depth) % depth, [to_core])
    experts(core * QUADS + far, mine, far)
    from_partner(far)
    partner_part(far)
    hand_over(far, 1)

    landed(from_core.at[first], core_sems.at[first])
    landed(from_core.at[sp], core_sems.at[sp])
    for step in back_steps:
        zz = (z + step) % depth
        landed(from_second.at[1, zz], second_sems.at[1, zz])
        mine[first, zz] = (
            f32(mine[first, zz]) + f32(from_core[first, zz]) + f32(from_second[1, zz])
        ).astype(jnp.bfloat16)
        send_back(mine.at[first, zz], from_first.at[zz], first_sems.at[zz], to_first)
    for step in back_steps:
        zz = (z + step) % depth
        landed(from_second.at[0, zz], second_sems.at[0, zz])
        landed(from_first.at[zz], first_sems.at[zz])
        total = (
            f32(mine[sp, zz])
            + f32(from_core[sp, zz])
            + f32(from_second[0, zz])
            + f32(from_first[zz])
        )
        if step:
            mine[sp, zz] = total.astype(jnp.bfloat16)
            send_back(mine.at[sp, zz], from_z.at[step - 1], z_sems.at[step - 1], to_z(step))
        else:
            total = resid[...] + total
            for slot in range(depth - 1):
                landed(from_z.at[slot], z_sems.at[slot])
                total = total + f32(from_z[slot])
            out_ref[...] = total.astype(out_ref.dtype)
    for copy in started + returned:
        copy.wait_send()


def heads_kernel(
    queries,
    keys,
    values,
    key_gates,
    query_gates,
    gain,
    stream,
    out_hbm,
    norm_gain,
    pieces,
    resid_out,
    rows_out,
    key_all,
    value_all,
    gate_all,
    peak,
    weight_total,
    weighted,
    leaving,
    incoming,
    out_w,
    local_sem,
    kv_send_sems,
    kv_recv_sems,
    out_send_sems,
    out_recv_sems,
):
    sp = lax.axis_index("sp")
    tp = lax.axis_index("tp")
    tp_count = lax.axis_size("tp")
    tokens = queries.shape[0]
    heads = queries.shape[1] // HD
    width = resid_out.shape[1]
    count = resid_out.shape[0]
    core = tp % 2
    x_next = sp + 1 - 2 * (sp % 2)
    y_next = (sp + 2) % 4
    first = x_next * (1 - core) + y_next * core
    second = y_next * (1 - core) + x_next * core
    far = 3 - sp
    load = pltpu.make_async_copy(out_hbm, out_w, local_sem.at[0])
    load.start()

    barrier = pltpu.get_barrier_semaphore()
    peers = [(first, tp), (second, tp)]
    peers += [(sp, (tp + step) % tp_count) for step in range(1, tp_count)]
    for peer in peers:
        pl.semaphore_signal(barrier, inc=1, device_id=peer, device_id_type=MESH)
    pl.semaphore_wait(barrier, len(peers))

    started = []

    def send_block(refs, quad, target):
        for part, (src, dst) in enumerate(zip(refs, (key_all, value_all, gate_all))):
            copy = pltpu.make_async_remote_copy(
                src_ref=src,
                dst_ref=dst.at[quad],
                send_sem=kv_send_sems.at[len(started)],
                recv_sem=kv_recv_sems.at[quad, part],
                device_id=target,
                device_id_type=MESH,
            )
            copy.start()
            started.append(copy)

    def block_of(quad):
        return (key_all.at[quad], value_all.at[quad], gate_all.at[quad])

    def receive_block(quad):
        for part, ref in enumerate(block_of(quad)):
            pltpu.make_async_remote_copy(
                src_ref=ref,
                dst_ref=ref,
                send_sem=kv_send_sems.at[0],
                recv_sem=kv_recv_sems.at[quad, part],
                device_id=(first, tp),
                device_id_type=MESH,
            ).wait_recv()

    chunk = 128

    def attend(refs, diagonal):
        key_ref, value_ref, gate_ref = refs

        @pl.loop(0, tokens // chunk)
        def _(j):
            rows = pl.ds(pl.multiple_of(j * chunk, chunk), chunk)
            for head in range(heads):
                cols = slice(head * HD, (head + 1) * HD)
                scores = lax.dot_general(
                    queries[rows, cols],
                    key_ref[:, cols],
                    (((1,), (1,)), ((), ())),
                    preferred_element_type=jnp.float32,
                )
                scores = (
                    scores * HD ** (-0.5)
                    + query_gates[rows, head : head + 1]
                    - gate_ref[head : head + 1, :]
                )
                if diagonal:
                    row_id = lax.broadcasted_iota(jnp.int32, scores.shape, 0) + j * chunk
                    col_id = lax.broadcasted_iota(jnp.int32, scores.shape, 1)
                    scores = jnp.where(col_id <= row_id, scores, masked_score)
                new_peak = jnp.max(scores, axis=1, keepdims=True)
                if not diagonal:
                    old_peak = peak[head, rows]
                    new_peak = jnp.maximum(old_peak, new_peak)
                lifted = jnp.exp(scores - new_peak)
                added = jnp.sum(lifted, axis=1, keepdims=True)
                product = jnp.dot(
                    lifted.astype(jnp.bfloat16),
                    value_ref[:, cols],
                    preferred_element_type=jnp.float32,
                )
                if not diagonal:
                    rescale = jnp.exp(old_peak - new_peak)
                    added = weight_total[head, rows] * rescale + added
                    product = weighted[head, rows] * rescale + product
                peak[head, rows] = new_peak
                weight_total[head, rows] = added
                weighted[head, rows] = product

    def attend_earlier(quad):
        @pl.when(quad < sp)
        def _():
            attend(block_of(quad), False)

    own = (keys, values, key_gates)
    send_block(own, sp, (first, tp))
    send_block(own, sp, (second, tp))
    attend(own, True)
    receive_block(first)
    send_block(block_of(first), first, (second, tp))
    attend_earlier(first)
    receive_block(second)
    attend_earlier(second)
    receive_block(far)
    attend_earlier(far)

    @pl.loop(0, tp_count)
    def _(j):
        rows = pl.ds(pl.multiple_of(j * count, count), count)
        for head in range(heads):
            cols = slice(head * HD, (head + 1) * HD)
            attended = weighted[head, rows] / weight_total[head, rows]
            square = jnp.mean(attended * attended, axis=1, keepdims=True)
            normed = attended * lax.rsqrt(square + 1e-06) * gain[0:1, cols]
            leaving[j, :, cols] = normed.astype(jnp.bfloat16)

    sent = []
    for step in range(1, tp_count):
        target = (tp + step) % tp_count
        copy = pltpu.make_async_remote_copy(
            src_ref=leaving.at[target],
            dst_ref=incoming.at[tp],
            send_sem=out_send_sems.at[step],
            recv_sem=out_recv_sems.at[tp],
            device_id=(sp, target),
            device_id_type=MESH,
        )
        copy.start()
        sent.append(copy)
    resid_out[...] = stream[...].astype(jnp.float32)
    load.wait()
    wide = heads * HD
    strip = 512 if width % 512 == 0 else width
    for step in range(tp_count):
        source = (tp - step + tp_count) % tp_count
        part = leaving if step == 0 else incoming
        if step:
            slot = incoming.at[source]
            pltpu.make_async_remote_copy(
                src_ref=slot,
                dst_ref=slot,
                send_sem=out_send_sems.at[0],
                recv_sem=out_recv_sems.at[source],
                device_id=(first, tp),
                device_id_type=MESH,
            ).wait_recv()

        @pl.loop(0, width // strip)
        def _(j):
            cols = pl.ds(pl.multiple_of(j * strip, strip), strip)
            weights = out_w[pl.ds(pl.multiple_of(source * wide, wide), wide), cols]
            resid_out[:, cols] += jnp.dot(
                part[source], weights, preferred_element_type=jnp.float32
            )

    resid = resid_out[...]
    center = resid - jnp.mean(resid, axis=1, keepdims=True)
    variance = jnp.mean(center * center, axis=1, keepdims=True)
    rows_out[:, :width] = (center * lax.rsqrt(variance + 1e-05) * norm_gain[0:1, :]).astype(
        jnp.bfloat16
    )
    rows_out[:, width:] = pieces[...]
    for copy in started + sent:
        copy.wait_send()


def weight_pieces(routing, route_weights):
    experts = jnp.arange(QUADS, dtype=jnp.int32)
    named = routing[:, :, None] == experts[None, None, :]
    weights = jnp.sum(jnp.where(named, route_weights[:, :, None], 0.0), axis=1)
    high = lax.reduce_precision(weights, 8, 7)
    middle = lax.reduce_precision(weights - high, 8, 7)
    low = weights - high - middle
    pieces = jnp.concatenate([high, middle, low], axis=1).astype(jnp.bfloat16)
    return jnp.pad(pieces, ((0, 0), (0, LANES - pieces.shape[1])))


def heads_stage(
    queries, keys, values, forget_totals, head_gain, stream, out_weight, norm_gain, pieces
):
    tokens, wide = queries.shape
    heads = wide // HD
    count, width = stream.shape
    tp_count = lax.axis_size("tp")
    key_gates = jnp.pad(jnp.transpose(forget_totals), ((0, (-heads) % 8), (0, 0)))
    bf16, f32 = jnp.bfloat16, jnp.float32
    dma = pltpu.SemaphoreType.DMA
    vmem = pl.BlockSpec(memory_space=pltpu.VMEM)
    hbm = pl.BlockSpec(memory_space=pl.ANY)
    return pl.pallas_call(
        heads_kernel,
        out_shape=(
            jax.ShapeDtypeStruct((count, width), f32),
            jax.ShapeDtypeStruct((count, width + LANES), bf16),
        ),
        in_specs=[vmem] * 7 + [hbm] + [vmem] * 2,
        out_specs=(vmem, vmem),
        scratch_shapes=[
            pltpu.VMEM((QUADS, tokens, wide), bf16),
            pltpu.VMEM((QUADS, tokens, wide), bf16),
            pltpu.VMEM((QUADS,) + key_gates.shape, f32),
            pltpu.VMEM((heads, tokens, 1), f32),
            pltpu.VMEM((heads, tokens, 1), f32),
            pltpu.VMEM((heads, tokens, HD), f32),
            pltpu.VMEM((tp_count, count, wide), bf16),
            pltpu.VMEM((tp_count, count, wide), bf16),
            pltpu.VMEM(out_weight.shape, bf16),
            dma((1,)),
            dma((9,)),
            dma((QUADS, 3)),
            dma((tp_count,)),
            dma((tp_count,)),
        ],
        compiler_params=pltpu.CompilerParams(
            collective_id=1, has_side_effects=True, vmem_limit_bytes=40 * 2**20
        ),
    )(
        queries,
        keys,
        values,
        key_gates,
        forget_totals,
        head_gain.reshape(1, -1),
        stream,
        out_weight,
        norm_gain.reshape(1, -1),
        pieces,
    )


def dense_experts(resid_sum, extended, gate_weight, up_weight, down_weight):
    depth = lax.axis_size("tp") // 2
    count, width = resid_sum.shape
    units = gate_weight.shape[2]
    bf16 = jnp.bfloat16
    dma = pltpu.SemaphoreType.DMA
    block = (depth, count, width)
    vmem = pl.BlockSpec(memory_space=pltpu.VMEM)
    hbm = pl.BlockSpec(memory_space=pl.ANY)
    ag_sends = (depth - 1 + 3) + 3 * (depth - 1) + 2 * depth + 2 * depth
    rs_sends = QUADS + 2 * depth + depth + depth - 1
    return pl.pallas_call(
        partial(experts_kernel, depth),
        out_shape=jax.ShapeDtypeStruct((count, width), bf16),
        in_specs=[vmem, vmem, hbm, hbm, hbm],
        out_specs=vmem,
        scratch_shapes=[
            pltpu.VMEM((2 * QUADS, depth, count, width + LANES), bf16),
            pltpu.VMEM((width, units), bf16),
            pltpu.VMEM((width, units), bf16),
            pltpu.VMEM((units, width), bf16),
            pltpu.VMEM((depth * count, units), bf16),
            pltpu.VMEM((QUADS,) + block, bf16),
            pltpu.VMEM((QUADS,) + block, bf16),
            pltpu.VMEM((QUADS,) + block, bf16),
            pltpu.VMEM((2,) + block, bf16),
            pltpu.VMEM(block, bf16),
            pltpu.VMEM((depth - 1, count, width), bf16),
            dma((4,)),
            dma((ag_sends,)),
            dma((2 * QUADS, depth)),
            dma((rs_sends,)),
            dma((QUADS,)),
            dma((2, depth)),
            dma((depth,)),
            dma((depth - 1,)),
        ],
        compiler_params=pltpu.CompilerParams(
            collective_id=0, has_side_effects=True, vmem_limit_bytes=48 * 2**20
        ),
    )(extended, resid_sum, gate_weight, up_weight, down_weight)


def routed_experts(
    resid_sum, normed_rows, routing, route_weights, gate_weight, up_weight, down_weight
):
    sp_count = lax.axis_size("sp")
    row_count = normed_rows.shape[0]
    capacity = max(2, 2 * TOP * row_count // sp_count)
    flat_expert = routing.reshape(-1)
    onehot = (flat_expert[:, None] == jnp.arange(sp_count, dtype=jnp.int32)[None, :]).astype(
        jnp.int32
    )
    earlier = jnp.cumsum(onehot, axis=0) - onehot
    slot_index = flat_expert * capacity + jnp.sum(earlier * onehot, axis=1)
    slot_grid = slot_index.reshape(row_count, TOP)
    slot_ids = jnp.arange(sp_count * capacity, dtype=jnp.int32)
    placing = jnp.sum(
        (slot_grid[None, :, :] == slot_ids[:, None, None]).astype(jnp.float32), axis=2
    ).astype(jnp.bfloat16)
    outgoing = jnp.dot(placing, normed_rows, preferred_element_type=jnp.float32).astype(
        jnp.bfloat16
    )
    outgoing = outgoing.reshape(sp_count, capacity, normed_rows.shape[1])
    arrived = lax.all_to_all(outgoing, "sp", split_axis=0, concat_axis=0, tiled=True)
    row_piece = lax.all_gather(arrived.reshape(-1, arrived.shape[2]), "tp", axis=0, tiled=True)
    gate_pre = jnp.dot(row_piece, gate_weight[0], preferred_element_type=jnp.float32)
    up_pre = jnp.dot(row_piece, up_weight[0], preferred_element_type=jnp.float32)
    hidden = (jax.nn.silu(gate_pre) * up_pre).astype(jnp.bfloat16)
    summed = lax.psum_scatter(
        jnp.dot(hidden, down_weight[0], preferred_element_type=jnp.float32).astype(jnp.bfloat16),
        "tp",
        scatter_dimension=0,
        tiled=True,
    )
    expert_out = summed.reshape(sp_count, capacity, -1)
    returned = lax.all_to_all(expert_out, "sp", split_axis=0, concat_axis=0, tiled=True)
    picked = returned.reshape(sp_count * capacity, -1)[slot_index].astype(jnp.float32)
    weighted = picked * route_weights.reshape(-1)[:, None]
    routed = jnp.sum(weighted.reshape(row_count, TOP, -1), axis=1)
    return (resid_sum + routed).astype(jnp.bfloat16)


def on_device(
    queries,
    key_vectors,
    value_vectors,
    forget_totals,
    head_gain,
    stream,
    out_weight,
    norm_gain,
    routing,
    route_weights,
    gate_weight,
    up_weight,
    down_weight,
):
    rows_dev, sp_size, tp_size = stream.shape[0], lax.axis_size("sp"), lax.axis_size("tp")
    dense = 2 * TOP * rows_dev // sp_size >= rows_dev
    if dense and sp_size == QUADS and tp_size % 4 == 0 and queries.shape[0] % 128 == 0:
        resid_sum, extended = heads_stage(
            queries,
            key_vectors,
            value_vectors,
            forget_totals,
            head_gain,
            stream,
            out_weight,
            norm_gain,
            weight_pieces(routing, route_weights),
        )
        return dense_experts(resid_sum, extended, gate_weight, up_weight, down_weight)
    tok_count = queries.shape[0]
    heads_dev = queries.shape[1] // HD
    sp_index = lax.axis_index("sp")
    sp_count = lax.axis_size("sp")
    gathered_gates = lax.all_gather(forget_totals, "sp", axis=0, tiled=True)
    first_pos = sp_index * tok_count
    query_pos = first_pos + jnp.arange(tok_count, dtype=jnp.int32)
    query_gate = jnp.transpose(lax.dynamic_slice_in_dim(gathered_gates, first_pos, tok_count, 0))
    segments = [(queries.reshape(tok_count, heads_dev, HD), query_gate, query_pos)]
    starting = (
        (
            jnp.full((heads_dev, tok_count), masked_score, jnp.float32),
            jnp.zeros((heads_dev, tok_count), jnp.float32),
            jnp.zeros((heads_dev, tok_count, HD), jnp.float32),
        ),
    )
    folder = make_folder(segments, gathered_gates)
    totals = folder(
        starting,
        (
            lax.all_gather(key_vectors, "sp", axis=0, tiled=True),
            lax.all_gather(value_vectors, "sp", axis=0, tiled=True),
        ),
        jnp.int32(0),
    )
    run_max, run_sum, run_acc = totals[0]
    attended = run_acc / run_sum[:, :, None]
    inverse_rms = lax.rsqrt(jnp.mean(attended * attended, axis=2, keepdims=True) + 1e-06)
    normed = attended * inverse_rms * head_gain.reshape(heads_dev, 1, HD)
    head_out = (
        jnp.transpose(normed, (1, 0, 2)).reshape(tok_count, heads_dev * HD).astype(jnp.bfloat16)
    )
    token_heads = lax.all_to_all(head_out, "tp", split_axis=0, concat_axis=1, tiled=True)
    mixed_rows = jnp.dot(token_heads, out_weight, preferred_element_type=jnp.float32)
    resid_sum = stream.astype(jnp.float32) + mixed_rows
    center = resid_sum - jnp.mean(resid_sum, axis=1, keepdims=True)
    normed_rows = (
        center * lax.rsqrt(jnp.mean(center * center, axis=1, keepdims=True) + 1e-05) * norm_gain
    ).astype(jnp.bfloat16)
    return routed_experts(
        resid_sum, normed_rows, routing, route_weights, gate_weight, up_weight, down_weight
    )


def solution(mesh):
    in_specs = (
        P("sp", "tp"),
        P("sp", "tp"),
        P("sp", "tp"),
        P("sp", "tp"),
        P("tp"),
        P(("sp", "tp"), None),
        P(),
        P(),
        P(("sp", "tp"), None),
        P(("sp", "tp"), None),
        P("sp", None, "tp"),
        P("sp", None, "tp"),
        P("sp", "tp", None),
    )
    out_specs = P(("sp", "tp"), None)
    return jax.shard_map(
        on_device, mesh=mesh, in_specs=in_specs, out_specs=out_specs, check_vma=False
    )
```
